32 devices in a mesh: ep: 8 (over z, y), tp: 4 (over x, core).
Axes of the slice: x: 2, y: 2, z: 4, core: 2. Of those that a mesh axis runs over, the one named last changes fastest.
Arguments:
- queries: bfloat16 [8192, 1024], P('ep', 'tp'), may hold values from -6 to 6
- key_rows: bfloat16 [8192, 256], P('ep', 'tp'), may hold values from -6 to 6
- values: bfloat16 [8192, 256], P('ep', 'tp'), may hold values from -6 to 6
- sink_logit: float32 [16], P('tp'), may hold values from 3 to 7
- out_weight: bfloat16 [1024, 2048], P('tp'), may hold values from -0.1875 to 0.1875
- out_gain: float32 [2048], replicated, may hold values from 0.1 to 1.9
- routed_tokens: bfloat16 [16384, 2048], P(('ep', 'tp')), may hold values from -6 to 6
- expert_ids: int32 [16384, 2], P(('ep', 'tp')), may hold values from 0 to 31, as said below
- route_weight: float32 [16384, 2], P(('ep', 'tp')), may hold values from 0.1 to 1
- routed_gain: float32 [2048], replicated, may hold values from 0.1 to 1.9
- expert_gate: bfloat16 [32, 2048, 1024], P('ep', None, 'tp'), may hold values from -0.125 to 0.125
- expert_up: bfloat16 [32, 2048, 1024], P('ep', None, 'tp'), may hold values from -0.125 to 0.125
- expert_down: bfloat16 [32, 2048, 1024], P('ep', None, 'tp'), may hold values from -0.1875 to 0.1875
Outputs:
- mixer_out: bfloat16 [8192, 2048], P(('ep', 'tp'))
- experts_out: bfloat16 [16384, 2048], P(('ep', 'tp'))
The draws below stay inside these ranges and needn't reach their ends.
Inputs may be any that keep to these rules, and one draw needn't show every extreme that they name: `expert_ids`: both experts of a row lie in one group (equal id // 8); the 512 rows of one device name every group exactly 512 / 4 times; the rows of one device name no expert more than 64 times; in every device's rows some expert of each group is named exactly 64 times, and one expert is named exactly 64 times by the rows of every device.
All inputs are finite; a program needn't handle non-finite values.
Results may differ from the reference program's by a relative error of at most 0.0071.
Values may be sent and summed in bfloat16 or wider, within the bound.
A program may use at most 192 MiB of HBM per device.

```python
import math
import jax
import jax.numpy as jnp
from jax import lax

D = 2048
HEADS = 16
KV_HEADS = 4
HEAD_DIM = 64
WINDOW = 128
QBLOCK = 512
EXPERTS = 32
GROUPS = 4
EPG = 8
TOP = 2
EXPERT_FF = 1024
TB = 512
CAP = 64
SEQ_A = 8192
TOKENS_B = 16384
N_EP = 8
N_TP = 4


def draw_queries(key, part):
    drawn = jax.random.normal(jax.random.fold_in(key, 12), (SEQ_A, HEADS * HEAD_DIM), jnp.float32)
    return jnp.clip(drawn, -4.0, 4.0).astype(jnp.bfloat16)


def draw_key_rows(key, part):
    drawn = jax.random.normal(jax.random.fold_in(key, 22), (SEQ_A, KV_HEADS * HEAD_DIM), jnp.float32)
    return jnp.clip(drawn, -4.0, 4.0).astype(jnp.bfloat16)


def draw_expert_ids(key, part):
    block_total = TOKENS_B // TB
    half_group = TB // (2 * GROUPS)
    common_hot = jax.random.randint(jax.random.fold_in(key, 101), (), 0, EPG)

    def one_block(block_index):
        block_key = jax.random.fold_in(jax.random.fold_in(key, 202), block_index)
        order_key, hot_key, rest_key = jax.random.split(block_key, 3)
        order = jax.random.permutation(order_key, TB)
        hottest = jax.random.randint(hot_key, (GROUPS,), 0, EPG).at[0].set(common_hot)
        others = jax.vmap(lambda inner: jax.random.permutation(inner, EPG - 1))(jax.random.split(rest_key, GROUPS))
        group = order % GROUPS
        rank = order // GROUPS
        hot_token = hottest[group]
        rest_token = others[group]
        stride = 1 + rank // (EPG - 1) % (EPG - 2)
        first_other = jnp.take_along_axis(rest_token, (rank % (EPG - 1))[:, None], axis=1)[:, 0]
        second_other = jnp.take_along_axis(rest_token, ((rank + stride) % (EPG - 1))[:, None], axis=1)[:, 0]
        other_one = (hot_token + 1 + first_other) % EPG
        other_two = (hot_token + 1 + second_other) % EPG
        leading = jnp.where(rank < half_group, hot_token, other_one)
        trailing = jnp.where(rank < half_group, other_one, other_two)
        return jnp.stack([group * EPG + leading, group * EPG + trailing], axis=-1)
    chosen = jax.vmap(one_block)(jnp.arange(block_total))
    return chosen.reshape(TOKENS_B, TOP).astype(jnp.int32)


def block_scale(rng, dims, shards, least, high):
    gain = 1.0
    for dim, blocks in shards:
        steps = jax.random.uniform(jax.random.fold_in(jax.random.fold_in(rng, 6), dim), (blocks,), jnp.float32, least / len(shards), high / len(shards))
        gain = gain * jnp.repeat(jnp.exp(steps), dims[dim] // blocks).reshape((-1,) + (1,) * (len(dims) - 1 - dim))
    return gain


def gaussian(rng, shape, deviation, most, cuts=(), kind=jnp.bfloat16):
    level = block_scale(rng, shape, cuts, -0.22, 0.18) if cuts else 1.0
    values = jax.random.normal(rng, shape, jnp.float32) * deviation * level
    return jnp.minimum(jnp.maximum(values, -most), most).astype(kind)


def setup_inputs(seed: int = 0) -> dict:
    seeds = jax.random.split(jax.random.key(seed), 14)
    queries = draw_queries(jax.random.fold_in(seeds[13], 71), 0)
    key_rows = draw_key_rows(jax.random.fold_in(seeds[13], 71), 0)
    values = gaussian(seeds[2], (SEQ_A, KV_HEADS * HEAD_DIM), 1.0, 6.0, ((0, 8), (1, 4)))
    sink_logit = jnp.clip(3.0 + 4.0 * jax.random.uniform(seeds[3], (HEADS,), jnp.float32) ** block_scale(seeds[3], (HEADS,), ((0, 4),), -0.2, 0.2), 3.0, 7.0)
    out_weight = gaussian(seeds[4], (HEADS * HEAD_DIM, D), (HEADS * HEAD_DIM) ** -0.5, 0.1875, ((0, 4),))
    out_gain = jnp.clip(1.0 + 0.18 * jax.random.normal(seeds[5], (D,), jnp.float32), 0.1, 1.9)
    routed_tokens = gaussian(seeds[6], (TOKENS_B, D), 1.0, 6.0, ((0, 32),))
    expert_ids = draw_expert_ids(jax.random.fold_in(seeds[13], 71), 0)
    route_weight = jnp.clip(jnp.exp(math.log(1.0) - 2.3025851 * jax.random.uniform(seeds[8], (TOKENS_B, TOP), jnp.float32) ** block_scale(seeds[8], (TOKENS_B, TOP), ((0, 32),), -0.2, 0.2)), 0.1, 1.0)
    routed_gain = jnp.clip(1.0 + 0.18 * jax.random.normal(seeds[9], (D,), jnp.float32), 0.1, 1.9)
    expert_gate = gaussian(seeds[10], (EXPERTS, D, EXPERT_FF), D ** -0.5, 0.125, ((0, 8), (2, 4)))
    expert_up = gaussian(seeds[11], (EXPERTS, D, EXPERT_FF), D ** -0.5, 0.125, ((0, 8), (2, 4)))
    expert_down = gaussian(seeds[12], (EXPERTS, D, EXPERT_FF), EXPERT_FF ** -0.5, 0.1875, ((0, 8), (2, 4)))
    return dict(queries=queries, key_rows=key_rows, values=values, sink_logit=sink_logit, out_weight=out_weight, out_gain=out_gain, routed_tokens=routed_tokens, expert_ids=expert_ids, route_weight=route_weight, routed_gain=routed_gain, expert_gate=expert_gate, expert_up=expert_up, expert_down=expert_down)


epsilon = 1e-06
far_below = -1e+30

def window_block(block_index, grouped, padded_keys, padded_values, sink_logit, seq_total):
    start_row = block_index * QBLOCK
    span_keys = QBLOCK + 2 * WINDOW
    query_block = lax.dynamic_slice_in_dim(grouped, start_row, QBLOCK, 0).astype(jnp.float32)
    key_block = lax.dynamic_slice_in_dim(padded_keys, start_row, span_keys, 0).astype(jnp.float32)
    value_block = lax.dynamic_slice_in_dim(padded_values, start_row, span_keys, 0).astype(jnp.float32)
    scores = jnp.einsum('qhgd,khd->hgqk', query_block, key_block) * HEAD_DIM ** (-0.5)
    query_pos = start_row + jnp.arange(QBLOCK, dtype=jnp.int32)
    key_pos = start_row - WINDOW + jnp.arange(span_keys, dtype=jnp.int32)
    valid = (jnp.abs(key_pos[None, :] - query_pos[:, None]) <= WINDOW) & (key_pos[None, :] >= 0) & (key_pos[None, :] < seq_total)
    sinks = sink_logit.reshape(KV_HEADS, HEADS // KV_HEADS)[:, :, None, None]
    masked = jnp.where(valid, scores, far_below)
    largest = jnp.maximum(lax.optimization_barrier(jnp.max(masked, axis=-1, keepdims=True)), sinks)
    raised = jnp.where(valid, jnp.exp(masked - largest), 0.0)
    denominator = lax.optimization_barrier(jnp.sum(raised, axis=-1, keepdims=True)) + jnp.exp(sinks - largest)
    weights = (raised / denominator).astype(jnp.bfloat16)
    attended = jnp.einsum('hgqk,khd->qhgd', weights.astype(jnp.float32), value_block)
    return attended.astype(jnp.bfloat16).reshape(QBLOCK, HEADS * HEAD_DIM)

def reference(queries, key_rows, values, sink_logit, out_weight, out_gain, routed_tokens, expert_ids, route_weight, routed_gain, expert_gate, expert_up, expert_down):
    seq_total = queries.shape[0]
    grouped = queries.reshape(seq_total, KV_HEADS, HEADS // KV_HEADS, HEAD_DIM)
    padding = ((WINDOW, WINDOW), (0, 0), (0, 0))
    padded_keys = jnp.pad(key_rows.reshape(seq_total, KV_HEADS, HEAD_DIM), padding)
    padded_values = jnp.pad(values.reshape(seq_total, KV_HEADS, HEAD_DIM), padding)
    block_ids = jnp.arange(seq_total // QBLOCK, dtype=jnp.int32)
    attended = lax.map(lambda block_index: window_block(block_index, grouped, padded_keys, padded_values, sink_logit, seq_total), block_ids)
    attended = attended.reshape(seq_total, HEADS * HEAD_DIM)
    mixed = jnp.dot(attended, out_weight, preferred_element_type=jnp.float32)
    mixer_out = (mixed * lax.rsqrt(lax.optimization_barrier(jnp.mean(mixed * mixed, axis=-1, keepdims=True)) + epsilon) * out_gain).astype(jnp.bfloat16)
    token_total = routed_tokens.shape[0]
    inputs = routed_tokens.astype(jnp.float32)
    normed = (inputs * lax.rsqrt(lax.optimization_barrier(jnp.mean(inputs * inputs, axis=-1, keepdims=True)) + epsilon) * routed_gain).astype(jnp.bfloat16)
    flat_ids = expert_ids.reshape(-1)
    most_rows = CAP * N_EP * N_TP
    empty = jnp.zeros((token_total * TOP, normed.shape[1]), jnp.bfloat16)

    def one_expert(results, expert):
        picked = jnp.nonzero(flat_ids == expert, size=most_rows, fill_value=token_total * TOP)[0]
        rows_in = jnp.take(normed, picked // TOP, axis=0, mode='fill', fill_value=0)
        gate = jnp.dot(rows_in, expert_gate[expert], preferred_element_type=jnp.float32)
        upward = jnp.dot(rows_in, expert_up[expert], preferred_element_type=jnp.float32)
        hidden = (jax.nn.silu(gate) * upward).astype(jnp.bfloat16)
        produced = jnp.dot(hidden, expert_down[expert].T, preferred_element_type=jnp.float32).astype(jnp.bfloat16)
        return (results.at[picked].set(produced, mode='drop'), None)
    results, unused = lax.scan(one_expert, empty, jnp.arange(EXPERTS, dtype=jnp.int32))
    results = results.reshape(token_total, TOP, normed.shape[1]).astype(jnp.float32)
    experts_out = lax.optimization_barrier(jnp.sum(results * route_weight[:, :, None], axis=1)).astype(jnp.bfloat16)
    return (mixer_out, experts_out)
```

```python
import functools

import jax
import jax.numpy as jnp
from jax import lax
from jax.experimental import pallas as pl
from jax.experimental.pallas import tpu as pltpu
from jax.sharding import Mesh, PartitionSpec as P

HEAD_DIM = 64
WINDOW = 128
QBLOCK = 512
EXPERTS = 32
EPG = 8
TOP = 2
GROUPS = EXPERTS // EPG
CHUNK_ROWS = 2048
ROW_TILE = 512

epsilon = 1e-06
EP = ("group", "member")
PLANE = ("member", "tp")


def padded(block, width):
    count = lax.axis_size(EP)
    forward = [(i, i + 1) for i in range(count - 1)]
    backward = [(target, source) for source, target in forward]
    low = lax.ppermute(block[-width:], EP, forward)
    high = lax.ppermute(block[:width], EP, backward)
    return jnp.concatenate([low, block, high], axis=0)


def attention(queries, key_rows, values, sink_logit, out_weight, out_gain):
    row_count = queries.shape[0]
    heads_here = queries.shape[1] // HEAD_DIM
    kv_here = key_rows.shape[1] // HEAD_DIM
    group_size = heads_here // kv_here
    full_weight = lax.all_gather(out_weight, "tp", axis=0, tiled=True)
    paired = jnp.concatenate((key_rows, values), axis=1)
    extended = padded(paired, WINDOW)
    offset = lax.axis_index(EP) * row_count
    seq_total = row_count * lax.axis_size(EP)
    grouped = queries.reshape(row_count, kv_here, group_size, HEAD_DIM)
    sinks = sink_logit.reshape(kv_here, group_size)[:, :, None, None]
    span_keys = QBLOCK + 2 * WINDOW

    def attend_block(block_index):
        start_row = block_index * QBLOCK
        query_block = lax.dynamic_slice_in_dim(grouped, start_row, QBLOCK, 0)
        band = lax.dynamic_slice_in_dim(extended, start_row, span_keys, 0)
        key_block = band[:, : kv_here * HEAD_DIM].reshape(span_keys, kv_here, HEAD_DIM)
        value_block = band[:, kv_here * HEAD_DIM :].reshape(span_keys, kv_here, HEAD_DIM)
        scores = jnp.einsum(
            "qhgd,khd->hgqk", query_block, key_block, preferred_element_type=jnp.float32
        ) * HEAD_DIM ** (-0.5)
        query_pos = offset + start_row + jnp.arange(QBLOCK, dtype=jnp.int32)
        key_pos = offset + start_row - WINDOW + jnp.arange(span_keys, dtype=jnp.int32)
        valid = (
            (jnp.abs(key_pos[None, :] - query_pos[:, None]) <= WINDOW)
            & (key_pos[None, :] >= 0)
            & (key_pos[None, :] < seq_total)
        )
        masked = jnp.where(valid, scores, -1e30)
        largest = jnp.maximum(jnp.max(masked, axis=-1, keepdims=True), sinks)
        raised = jnp.where(valid, jnp.exp(masked - largest), 0.0)
        denominator = jnp.sum(raised, axis=-1, keepdims=True) + jnp.exp(sinks - largest)
        weights = (raised / denominator).astype(jnp.bfloat16)
        attended = jnp.einsum(
            "hgqk,khd->qhgd", weights, value_block, preferred_element_type=jnp.float32
        )
        return attended.astype(jnp.bfloat16).reshape(QBLOCK, heads_here * HEAD_DIM)

    attended = lax.map(attend_block, jnp.arange(row_count // QBLOCK, dtype=jnp.int32))
    attended = attended.reshape(row_count, heads_here * HEAD_DIM)
    attended = lax.all_to_all(attended, "tp", split_axis=0, concat_axis=1, tiled=True)
    mixed = jnp.dot(attended, full_weight, preferred_element_type=jnp.float32)
    return (
        mixed * lax.rsqrt(jnp.mean(mixed * mixed, axis=-1, keepdims=True) + epsilon) * out_gain
    ).astype(jnp.bfloat16)


def expert_kernel(x_ref, w_ref, gate_ref, up_ref, down_ref, out_ref, total):
    x = x_ref[...]
    for e in range(gate_ref.shape[0]):
        gate = jnp.dot(x, gate_ref[e], preferred_element_type=jnp.float32)
        upward = jnp.dot(x, up_ref[e], preferred_element_type=jnp.float32)
        hidden = (gate / (1.0 + jnp.exp(-gate)) * upward * w_ref[:, e : e + 1]).astype(
            jnp.bfloat16
        )
        part = lax.dot_general(
            hidden, down_ref[e], (((1,), (1,)), ((), ())), preferred_element_type=jnp.float32
        )
        if e == 0:
            total[...] = part
        else:
            total[...] += part
    out_ref[...] = total[...].astype(jnp.bfloat16)


def apply_experts(rows, weights, gate, up, down):
    count, width = rows.shape
    local_experts, _, units = gate.shape
    tile = min(ROW_TILE, count)
    whole = lambda i: (0, 0, 0)
    return pl.pallas_call(
        expert_kernel,
        grid=(count // tile,),
        out_shape=jax.ShapeDtypeStruct((count, width), jnp.bfloat16),
        in_specs=[
            pl.BlockSpec((tile, width), lambda i: (i, 0)),
            pl.BlockSpec((tile, local_experts), lambda i: (i, 0)),
            pl.BlockSpec(gate.shape, whole, pipeline_mode=pl.Buffered(1)),
            pl.BlockSpec(up.shape, whole, pipeline_mode=pl.Buffered(1)),
            pl.BlockSpec(down.shape, whole, pipeline_mode=pl.Buffered(1)),
        ],
        out_specs=pl.BlockSpec((tile, width), lambda i: (i, 0)),
        scratch_shapes=[pltpu.VMEM((tile, width), jnp.float32)],
        compiler_params=pltpu.CompilerParams(vmem_limit_bytes=48 * 2**20),
        cost_estimate=pl.CostEstimate(
            flops=6 * count * width * local_experts * units,
            bytes_accessed=4 * count * width + 6 * local_experts * units * width,
            transcendentals=count * local_experts * units,
        ),
    )(rows, weights, gate, up, down)


def routed(tokens, expert_ids, route_weight, gain, gate, up, down):
    token_total, width = tokens.shape
    share = token_total // GROUPS
    plane = lax.axis_size(PLANE)
    local_experts = gate.shape[0]
    inputs = tokens.astype(jnp.float32)
    normed = (
        inputs * lax.rsqrt(jnp.mean(inputs * inputs, axis=-1, keepdims=True) + epsilon) * gain
    ).astype(jnp.bfloat16)
    group = expert_ids[:, 0] // EPG
    in_group = (group[:, None] == jnp.arange(GROUPS, dtype=jnp.int32)).astype(jnp.float32)
    index = jnp.arange(token_total, dtype=jnp.int32)
    before = (index[None, :] < index[:, None]).astype(jnp.float32)
    ranks = jnp.dot(before, in_group, preferred_element_type=jnp.float32)
    rank = jnp.sum(ranks * in_group, axis=1).astype(jnp.int32)
    position = group * share + rank
    order = (position[None, :] == index[:, None]).astype(jnp.bfloat16)
    back = (position[:, None] == index[None, :]).astype(jnp.bfloat16)
    ordered = jnp.dot(order, normed, preferred_element_type=jnp.float32).astype(jnp.bfloat16)
    member = jnp.arange(EPG, dtype=jnp.int32)
    spread = jnp.sum(
        jnp.where((expert_ids % EPG)[:, :, None] == member, route_weight[:, :, None], 0.0), axis=1
    )
    spread = jnp.dot(
        order.astype(jnp.float32), spread, precision=lax.Precision.HIGHEST,
        preferred_element_type=jnp.float32,
    )
    spread = spread.reshape(GROUPS, share, EPG).transpose(0, 2, 1).reshape(GROUPS, EPG * share)
    spread = lax.all_to_all(spread, "group", 0, 0, tiled=True)
    spread = lax.all_gather(spread, PLANE, axis=0, tiled=True)
    spread = spread.reshape(plane, GROUPS, EPG, share)
    mine = lax.dynamic_slice_in_dim(
        spread, lax.axis_index("member") * local_experts, local_experts, 2
    ).transpose(0, 1, 3, 2)
    piece = max(min(share, CHUNK_ROWS // (plane * GROUPS)), 16)
    ordered = ordered.reshape(GROUPS, share, width)
    results = []
    for start in range(0, share, piece):
        sent = lax.all_to_all(ordered[:, start : start + piece], "group", 0, 0, tiled=True)
        sent = sent.reshape(GROUPS * piece, width)
        rows = lax.all_gather(sent, PLANE, axis=0, tiled=True)
        weights = mine[:, :, start : start + piece].reshape(plane * GROUPS * piece, local_experts)
        partial = apply_experts(rows, weights, gate, up, down)
        summed = lax.psum_scatter(partial, PLANE, scatter_dimension=0, tiled=True)
        summed = summed.reshape(GROUPS, piece, width)
        results.append(lax.all_to_all(summed, "group", 0, 0, tiled=True))
    result = jnp.concatenate(results, axis=1).reshape(token_total, width)
    return jnp.dot(back, result, preferred_element_type=jnp.float32).astype(jnp.bfloat16)


def local(queries, key_rows, values, sink_logit, out_weight, out_gain, routed_tokens,
          expert_ids, route_weight, routed_gain, expert_gate, expert_up, expert_down):
    experts_out = routed(
        routed_tokens, expert_ids, route_weight, routed_gain, expert_gate, expert_up, expert_down
    )
    mixer_out = attention(queries, key_rows, values, sink_logit, out_weight, out_gain)
    return (mixer_out, experts_out)


def solution(mesh):
    ep, tp = mesh.shape["ep"], mesh.shape["tp"]
    split = Mesh(mesh.devices.reshape(GROUPS, ep // GROUPS, tp), ("group", "member", "tp"))
    every = ("group", "member", "tp")
    placed = (
        P(EP, "tp"),
        P(EP, "tp"),
        P(EP, "tp"),
        P("tp"),
        P("tp", None),
        P(),
        P(every, None),
        P(every, None),
        P(every, None),
        P(),
        P(EP, None, "tp"),
        P(EP, None, "tp"),
        P(EP, None, "tp"),
    )
    return jax.shard_map(
        local,
        mesh=split,
        in_specs=placed,
        out_specs=(P(every, None), P(every, None)),
        check_vma=False,
    )
```
